32 devices in a mesh: sp: 8 (over z, x), tp: 4 (over y, core).
Axes of the slice: x: 2, y: 2, z: 4, core: 2. Of those that a mesh axis runs over, the one named last changes fastest.
Arguments:
- queries: bfloat16 [5120, 2048], P('sp', 'tp'), may hold values from -164 to 164
- keys: bfloat16 [5120, 512], P('sp', 'tp'), may hold values from -6 to 6
- values: bfloat16 [5120, 512], P('sp', 'tp'), may hold values from -6 to 6
- sink: float32 [32], P('tp'), may hold values from 4 to 8
- stream: bfloat16 [5120, 2048], P(('sp', 'tp')), may hold values from -6 to 6
- out_weight: bfloat16 [2048, 2048], P('tp'), may hold values from -0.5390625 to 0.5390625
- norm_gain: float32 [2048], replicated, may hold values from 0.1 to 1.9
- gate_weight: bfloat16 [2048, 5632], P('sp', 'tp'), may hold values from -0.125 to 0.125
- up_weight: bfloat16 [2048, 5632], P('sp', 'tp'), may hold values from -0.125 to 0.125
- down_weight: bfloat16 [5632, 2048], P('tp', 'sp'), may hold values from -0.23925781 to 0.23925781
Outputs:
- result: bfloat16 [5120, 2048], P(('sp', 'tp'))
The draws below stay inside these ranges and needn't reach their ends.
All inputs are finite; a program needn't handle non-finite values.
Results may differ from the reference program's by a relative error of at most 0.019.
Values may be sent and summed in bfloat16 or wider, within the bound.
A program may use at most 128 MiB of HBM per device.

```python
import jax
import jax.numpy as jnp
from jax import lax

D = 2048
HEADS = 32
KV_HEADS = 8
HEAD = 64
FF = 5632
WINDOW = 128
TOK_DEV = 640
TOKENS = 5120


def draw_queries(key, part):
    shape = (TOKENS, HEADS * HEAD)
    return jnp.clip(2.0 * jax.random.normal(key, shape, jnp.float32), -12.0, 12.0).astype(jnp.bfloat16)


def block_scale(key, shape, cuts, least, largest):
    def one(axis_at, shards_of):
        steps = jax.random.uniform(jax.random.fold_in(jax.random.fold_in(key, 6), axis_at), (shards_of,), jnp.float32, least / len(cuts), largest / len(cuts))
        return jnp.repeat(jnp.exp(steps), shape[axis_at] // shards_of).reshape((-1,) + (1,) * (len(shape) - axis_at - 1))

    gain = one(*cuts[0])
    for cut in cuts[1:]:
        gain = gain * one(*cut)
    return gain


def normal_values(own_key, extent, width, bound, cuts=(), held_as=jnp.bfloat16):
    level = block_scale(own_key, extent, cuts, -0.22, 0.18) if cuts else 1.0
    array = jax.random.normal(own_key, extent, jnp.float32) * width * level
    return jnp.minimum(jnp.maximum(array, -bound), bound).astype(held_as)


def setup_inputs(seed: int = 0) -> dict:
    key_list = jax.random.split(jax.random.key(seed), 11)
    return {
        "queries": draw_queries(jax.random.fold_in(key_list[10], 71), 0),
        "keys": normal_values(key_list[1], (TOKENS, KV_HEADS * HEAD), 1.0, 6.0, ((0, 8), (1, 4))),
        "values": normal_values(key_list[2], (TOKENS, KV_HEADS * HEAD), 1.0, 6.0, ((0, 8), (1, 4))),
        "sink": jnp.clip(4.0 + 4.0 * jax.random.uniform(key_list[3], (HEADS,), jnp.float32) ** block_scale(key_list[3], (HEADS,), ((0, 4),), -0.2, 0.2), 4.0, 8.0),
        "stream": normal_values(key_list[4], (TOKENS, D), 1.0, 6.0, ((0, 32),)),
        "out_weight": normal_values(key_list[5], (HEADS * HEAD, D), 0.09, 0.5390625, ((0, 4),)),
        "norm_gain": jnp.clip(1.0 + 0.18 * jax.random.normal(key_list[6], (D,), jnp.float32), 0.1, 1.9),
        "gate_weight": normal_values(key_list[7], (D, FF), D ** -0.5, 0.125, ((0, 8), (1, 4))),
        "up_weight": normal_values(key_list[8], (D, FF), D ** -0.5, 0.125, ((0, 8), (1, 4))),
        "down_weight": normal_values(key_list[9], (FF, D), 0.04, 0.23925781, ((0, 4), (1, 8))),
    }


def rotary(block, start):
    length = block.shape[0]
    middle = HEAD // 2
    inverse = 1.0 / 10000.0 ** (jnp.arange(0, HEAD, 2, dtype=jnp.float32) / HEAD)
    places = (start + jnp.arange(length, dtype=jnp.int32)).astype(jnp.float32)
    angles = places[:, None, None] * inverse[None, None, :]
    cosine_table = jnp.cos(angles)
    sine_table = jnp.sin(angles)
    pieces = block.astype(jnp.float32).reshape(length, -1, HEAD)
    leading = pieces[..., :middle]
    trailing = pieces[..., middle:]
    turned = jnp.concatenate([leading * cosine_table - trailing * sine_table, trailing * cosine_table + leading * sine_table], -1)
    return turned.reshape(length, -1).astype(jnp.bfloat16)

def reference(queries, keys, values, sink, stream, out_weight, norm_gain, gate_weight, up_weight, down_weight):
    length = queries.shape[0]
    blocks = length // WINDOW
    group = HEADS // KV_HEADS
    kv_width = KV_HEADS * HEAD
    turned_q = rotary(queries, 0)
    turned_k = rotary(keys, 0)
    paired = jnp.concatenate([turned_k, values], 1)
    padded = jnp.pad(paired, ((WINDOW, WINDOW), (0, 0)))
    framed = padded.reshape(blocks + 2, WINDOW, 2 * kv_width)
    banded = jnp.concatenate([framed[:-2], framed[1:-1], framed[2:]], axis=1)
    key_band = jnp.moveaxis(banded[..., :kv_width].reshape(blocks, 3 * WINDOW, KV_HEADS, HEAD), 2, 0)
    value_band = jnp.moveaxis(banded[..., kv_width:].reshape(blocks, 3 * WINDOW, KV_HEADS, HEAD), 2, 0)
    query_blocks = jnp.moveaxis(turned_q.reshape(blocks, WINDOW, KV_HEADS, group, HEAD), 2, 0)
    sink_grid = sink.reshape(KV_HEADS, group)
    query_place = jnp.arange(blocks)[:, None, None] * WINDOW + jnp.arange(WINDOW)[None, :, None]
    key_place = jnp.arange(blocks)[:, None, None] * WINDOW - WINDOW + jnp.arange(3 * WINDOW)[None, None, :]
    valid = (jnp.abs(key_place - query_place) <= WINDOW) & (key_place >= 0) & (key_place < length)

    def one_head(item):
        query_part, key_part, value_part, sink_part = item
        scores = jnp.einsum('nqgd,nsd->ngqs', query_part.astype(jnp.float32), key_part.astype(jnp.float32)) * HEAD ** (-0.5)
        scores = jnp.where(valid[:, None], scores, -jnp.inf)
        sink_here = sink_part[None, :, None]
        top = jnp.maximum(lax.optimization_barrier(jnp.max(scores, -1)), sink_here)
        raised = jnp.exp(scores - top[..., None])
        denom = lax.optimization_barrier(jnp.sum(raised, -1)) + jnp.exp(sink_here - top)
        weights = lax.optimization_barrier((raised / denom[..., None]).astype(jnp.bfloat16))
        output = jnp.einsum('ngqs,nsd->nqgd', weights.astype(jnp.float32), value_part.astype(jnp.float32))
        return output.astype(jnp.bfloat16)
    heads_out = lax.map(one_head, (query_blocks, key_band, value_band, sink_grid))
    attended = jnp.moveaxis(heads_out, 0, 2).reshape(length, HEADS * HEAD)
    mixed = (stream.astype(jnp.float32) + jnp.dot(attended, out_weight, preferred_element_type=jnp.float32)).astype(jnp.bfloat16)
    mixed_wide = mixed.astype(jnp.float32)
    scale = lax.rsqrt(lax.optimization_barrier(jnp.mean(mixed_wide * mixed_wide, -1, keepdims=True)) + 1e-06)
    normed = (mixed_wide * scale * norm_gain).astype(jnp.bfloat16)

    def feed_forward(rows):
        gate = jnp.dot(rows, gate_weight, preferred_element_type=jnp.float32)
        upward = jnp.dot(rows, up_weight, preferred_element_type=jnp.float32)
        hidden = (jax.nn.silu(gate) * upward).astype(jnp.bfloat16)
        return jnp.dot(hidden, down_weight, preferred_element_type=jnp.float32)
    lowered = lax.map(feed_forward, normed.reshape(-1, TOK_DEV, D)).reshape(length, D)
    return (mixed_wide + 0.5 * lowered).astype(jnp.bfloat16)
```

```python
import functools

import jax
import jax.numpy as jnp
import numpy as np
from jax import lax
from jax.experimental import pallas as pl
from jax.experimental.pallas import tpu as pltpu
from jax.sharding import PartitionSpec as P

HEAD = 64
WINDOW = 128
LANES = 128
BF = jnp.bfloat16
F32 = jnp.float32
MESH = pl.DeviceIdType.MESH


def padded_2(cells, sides, width):
    for axis, dim in sides:
        count = lax.axis_size(axis)
        ends = count - 1
        head = lax.slice_in_dim(cells, 0, width, axis=dim)
        tail = lax.slice_in_dim(cells, cells.shape[dim] - width, cells.shape[dim], axis=dim)
        cells = jnp.concatenate(
            [
                lax.ppermute(tail, axis, [(i, (i + 1) % count) for i in range(ends)]),
                cells,
                lax.ppermute(head, axis, [((i + 1) % count, i) for i in range(ends)]),
            ],
            axis=dim,
        )
    return cells


def rotary(block, start):
    length = block.shape[0]
    middle = HEAD // 2
    inverse = 1.0 / 10000.0 ** (jnp.arange(0, HEAD, 2, dtype=jnp.float32) / HEAD)
    places = (start + jnp.arange(length, dtype=jnp.int32)).astype(jnp.float32)
    angles = places[:, None, None] * inverse[None, None, :]
    cosine_table = jnp.cos(angles)
    sine_table = jnp.sin(angles)
    pieces = block.astype(jnp.float32).reshape(length, -1, HEAD)
    leading = pieces[..., :middle]
    trailing = pieces[..., middle:]
    turned = jnp.concatenate(
        [
            leading * cosine_table - trailing * sine_table,
            trailing * cosine_table + leading * sine_table,
        ],
        -1,
    )
    return turned.reshape(length, -1).astype(jnp.bfloat16)


def window_attend(queries, keys, values, sink):
    rows_here = queries.shape[0]
    start = lax.axis_index("sp") * rows_here
    length = lax.axis_size("sp") * rows_here
    blocks = rows_here // WINDOW
    kv_width = keys.shape[1]
    kv_count = kv_width // HEAD
    head_count = queries.shape[1] // HEAD
    group = head_count // kv_count
    turned_q = rotary(queries, start)
    turned_k = rotary(keys, start)
    paired = jnp.concatenate([turned_k, values], 1)
    padded = padded_2(paired, (("sp", 0),), WINDOW)
    framed = padded.reshape(blocks + 2, WINDOW, 2 * kv_width)
    banded = jnp.concatenate([framed[:-2], framed[1:-1], framed[2:]], axis=1)
    key_band = banded[..., :kv_width].reshape(blocks, 3 * WINDOW, kv_count, HEAD)
    value_band = banded[..., kv_width:].reshape(blocks, 3 * WINDOW, kv_count, HEAD)
    query_blocks = turned_q.reshape(blocks, WINDOW, kv_count, group, HEAD)
    scores = jnp.einsum(
        "nqkgd,nskd->nkgqs", query_blocks, key_band, preferred_element_type=jnp.float32
    ) * HEAD ** (-0.5)
    query_place = (
        start + jnp.arange(blocks)[:, None, None] * WINDOW + jnp.arange(WINDOW)[None, :, None]
    )
    key_place = (
        start
        + jnp.arange(blocks)[:, None, None] * WINDOW
        - WINDOW
        + jnp.arange(3 * WINDOW)[None, None, :]
    )
    valid = (jnp.abs(key_place - query_place) <= WINDOW) & (key_place >= 0) & (key_place < length)
    scores = jnp.where(valid[:, None, None], scores, -jnp.inf)
    sink_grid = sink.reshape(kv_count, group)[None, :, :, None]
    top = jnp.maximum(jnp.max(scores, -1), sink_grid)
    raised = jnp.exp(scores - top[..., None])
    denom = jnp.sum(raised, -1) + jnp.exp(sink_grid - top)
    weights = (raised / denom[..., None]).astype(jnp.bfloat16)
    output = jnp.einsum(
        "nkgqs,nskd->nqkgd", weights, value_band, preferred_element_type=jnp.float32
    )
    return output.astype(jnp.bfloat16).reshape(rows_here, head_count * HEAD)


def collect_weights(gate_weight, up_weight, down_weight):
    return (
        lax.all_gather(gate_weight, "sp", axis=0, tiled=True),
        lax.all_gather(up_weight, "sp", axis=0, tiled=True),
        lax.all_gather(down_weight, "sp", axis=1, tiled=True),
    )


def local(
    queries, keys, values, sink, stream, out_weight, norm_gain, gate_weight, up_weight, down_weight
):
    attended = window_attend(queries, keys, values, sink)
    gathered = collect_weights(gate_weight, up_weight, down_weight)
    gate_whole, up_whole, down_whole = gathered
    rows = attended
    projected = lax.psum_scatter(
        jnp.dot(rows, out_weight, preferred_element_type=jnp.float32),
        "tp",
        scatter_dimension=0,
        tiled=True,
    )
    mixed = (stream.astype(jnp.float32) + projected).astype(jnp.bfloat16)
    mixed_wide = mixed.astype(jnp.float32)
    scale = lax.rsqrt(jnp.mean(mixed_wide * mixed_wide, -1, keepdims=True) + 1e-06)
    normed = (mixed_wide * scale * norm_gain).astype(jnp.bfloat16)
    piece = lax.all_gather(normed, "tp", axis=0, tiled=True)
    gate = jnp.dot(piece, gate_whole, preferred_element_type=jnp.float32)
    upward = jnp.dot(piece, up_whole, preferred_element_type=jnp.float32)
    hidden = (jax.nn.silu(gate) * upward).astype(jnp.bfloat16)
    rows = hidden
    lowered = lax.psum_scatter(
        jnp.dot(rows, down_whole, preferred_element_type=jnp.float32).astype(jnp.bfloat16),
        "tp",
        scatter_dimension=0,
        tiled=True,
    ).astype(jnp.float32)
    return (mixed_wide + 0.5 * lowered).astype(jnp.bfloat16)


def turn_tables(blocks):
    lane = np.arange(LANES)
    inverse = 10000.0 ** (-2.0 * (lane % (HEAD // 2)) / HEAD)
    within = np.arange(WINDOW)[:, None] * inverse[None, :]
    begins = (np.arange(blocks) - 1)[:, None] * WINDOW * inverse[None, :]
    pair = lambda a: np.stack([np.cos(a), np.sin(a)]).astype(np.float32)
    return pair(within), pair(begins)


NAMES = "onfs"
GCH, DCH = 4, 4


def layer_kernel(
    dims, q_in, k_in, v_in, sink_ref, stream_in, w_in, gain_ref, gate_in, up_in, down_in, turn_ref, begin_ref,
    out_ref,
    qv, kv, kk, vv, att, wv, sv, tails, oth, doth, gu, dn, p_send, p_recv, kept, y_send, y_recv, mixed, nt,
    hid, c_send, c_recv, acc, s1, r1, s2, r2,
    loc, h_ss, h_rs, z_ss, x_ss, gu_rs, d_rs, p_ss, p_rs, n_ss, n_rs, e_ss, e_rs,
):
    length, tokens, rows, per, tail, total = dims
    s = lax.axis_index("sp")
    z, x = s // 2, s % 2
    t = lax.axis_index("tp")
    y, c = t // 2, t % 2
    part = z % 2
    pz = z + 1 - 2 * part
    half = length // 2
    flip = lambda q: q + half - 2 * half * (q // half)
    fz, fp = flip(z), flip(pz)
    dests = {"o": fz, "n": pz, "f": fp, "s": z}
    outer = (z == 0) | (z == length - 1)
    at_x = {"sp": s + 1 - 2 * x}
    at_n = {"sp": 2 * pz + x}
    at_y = {"tp": t + 2 - 4 * y}
    at_c = {"tp": t + 1 - 2 * c}
    last = 2 * length - 1
    model = out_ref.shape[1]
    blocks = tokens // WINDOW
    edge = per * 2 * LANES
    cut = per * LANES

    def send(src, dst, ssem, rsem, to):
        return pltpu.make_async_remote_copy(
            src_ref=src, dst_ref=dst, send_sem=ssem, recv_sem=rsem,
            device_id=to, device_id_type=MESH,
        )

    def fetch(src, dst, i):
        return pltpu.make_async_copy(src, dst, loc.at[i])

    def fetch_part(which, dst, i):
        for n in range(per):
            at = pl.multiple_of((which * per + n) * LANES, LANES)
            for side, src in ((0, gate_in), (1, up_in)):
                fetch(src.at[:, pl.ds(at, LANES)], dst.at[:, pl.ds((2 * n + side) * LANES, LANES)], i).start()

    def fetch_down(which, dst, i):
        fetch(down_in.at[pl.ds(pl.multiple_of(which * cut, LANES), cut)], dst.at[pl.ds(0, cut)], i).start()
        at = pl.multiple_of(edge + which * tail, tail)
        fetch(down_in.at[pl.ds(at, tail)], dst.at[pl.ds(cut, tail)], i).start()

    whole_k = fetch(k_in, kv.at[pl.ds(WINDOW, tokens), pl.ds(0, LANES)], 3)
    whole_v = fetch(v_in, kv.at[pl.ds(WINDOW, tokens), pl.ds(LANES, LANES)], 4)
    whole_q = fetch(q_in, qv, 5)
    whole_w = fetch(w_in, wv, 8)
    whole_s = fetch(stream_in, sv, 9)
    fetch_part(1 - part, oth, 0)
    fetch(gate_in.at[:, pl.ds(edge, LANES)], tails.at[0], 2).start()
    fetch(up_in.at[:, pl.ds(edge, LANES)], tails.at[1], 2).start()
    fetch_part(part, gu.at[s], 1)
    whole_k.start()
    whole_v.start()
    fetch_down(1 - part, doth, 7)
    whole_q.start()
    fetch_down(part, dn.at[s], 6)
    whole_w.start()
    whole_s.start()

    barrier = pltpu.get_barrier_semaphore()

    def greet(to):
        pl.semaphore_signal(barrier, inc=1, device_id=to, device_id_type=MESH)

    for to in (at_x, at_n, {"sp": 2 * fz + x}, {"sp": 2 * fp + x}, at_y, at_c):
        greet(to)
    hop_up = (x == 1) & (z < length - 1)
    hop_down = (x == 0) & (z > 0)
    pl.when(hop_up)(lambda: greet({"sp": s + 1}))
    pl.when(hop_down)(lambda: greet({"sp": s - 1}))
    pl.semaphore_wait(barrier, 6 + hop_up.astype(jnp.int32) + hop_down.astype(jnp.int32))

    halos = []
    for i, src in ((0, k_in), (1, v_in)):
        cols = pl.ds(i * LANES, LANES)
        after = send(src.at[pl.ds(tokens - WINDOW, WINDOW)], kv.at[pl.ds(0, WINDOW), cols], h_ss.at[0, i], h_rs.at[0, i], {"sp": s + 1})
        before = send(src.at[pl.ds(0, WINDOW)], kv.at[pl.ds(tokens + WINDOW, WINDOW), cols], h_ss.at[1, i], h_rs.at[1, i], {"sp": s - 1})
        pl.when(s < last)(after.start)
        pl.when(s > 0)(before.start)
        halos.append((after, before))

    chunks = (GCH, DCH)

    def piece(kind, ref, g):
        size = (gu, dn)[kind].shape[1] // chunks[kind]
        return ref.at[pl.ds(g * size, size)]

    def slot_of(name):
        return 2 * dests[name] + x

    def buffers(kind):
        return ((gu, gu_rs), (dn, d_rs))[kind]

    def by_z(kind, name, g):
        buf, got = buffers(kind)
        src = buf.at[s] if name == "o" else (oth, doth)[kind]
        sem = z_ss.at[kind, NAMES.index(name), g]
        return send(piece(kind, src, g), piece(kind, buf.at[s], g), sem, got.at[s, g], {"sp": slot_of(name)})

    def by_x(kind, name, g):
        buf, got = buffers(kind)
        here = piece(kind, buf.at[slot_of(name)], g)
        return send(here, here, x_ss.at[kind, NAMES.index(name), g], got.at[slot_of(name), g], at_x)

    def landed(kind, slot, g):
        buf, got = buffers(kind)
        here = piece(kind, buf.at[slot], g)
        send(here, here, x_ss.at[0, 0, 0], got.at[slot, g], at_x).wait_recv()

    def push(kind, name):
        for g in range(chunks[kind]):
            by_z(kind, name, g).start()

    def relay(kind, name, some=None):
        for g in range(chunks[kind]) if some is None else some:
            if name != "s":
                landed(kind, slot_of(name), g)
            by_x(kind, name, g).start()

    def crossed(kind, name):
        for g in range(chunks[kind]):
            landed(kind, 2 * dests[name] + 1 - x, g)

    fetch(oth.at[:, pl.ds(0, edge)], oth.at[:, pl.ds(0, edge)], 0).wait()
    fetch(tails, tails, 2).wait()
    low_tail = jnp.concatenate([tails[0, :, :tail], tails[1, :, :tail]], 1)
    high_tail = jnp.concatenate([tails[0, :, tail:], tails[1, :, tail:]], 1)
    oth[:, edge:] = jnp.where(part == 0, high_tail, low_tail)
    gu[s, :, edge:] = jnp.where(part == 0, low_tail, high_tail)
    push(0, "n")
    own = gu.at[s, :, pl.ds(0, edge)]
    fetch(own, own, 1).wait()
    relay(0, "s")
    fetch(doth, doth, 7).wait()
    push(1, "n")
    push(0, "o")
    pl.when(jnp.logical_not(outer))(lambda: push(0, "f"))
    fetch(dn.at[s], dn.at[s], 6).wait()

    lane = lax.broadcasted_iota(jnp.int32, (WINDOW, LANES), 1)
    low = lane < HEAD
    front = lane % HEAD < HEAD // 2

    def angles(m):
        row = s * blocks + m
        cos_b, sin_b = begin_ref[0, pl.ds(row, 1), :], begin_ref[1, pl.ds(row, 1), :]
        cosine = turn_ref[0] * cos_b - turn_ref[1] * sin_b
        sine = turn_ref[1] * cos_b + turn_ref[0] * sin_b
        return cosine, jnp.where(front, -sine, sine)

    def turned(block, cosine, sine):
        cells = block.astype(F32)
        other = jnp.where(front, pltpu.roll(cells, LANES - HEAD // 2, 1), pltpu.roll(cells, HEAD // 2, 1))
        return cells * cosine + other * sine

    def spread(m, carry):
        at = pl.ds(pl.multiple_of(m * WINDOW, WINDOW), WINDOW)
        cosine, sine = angles(m)
        for cells, dst in ((turned(kv[at, :LANES], cosine, sine), kk), (kv[at, LANES:].astype(F32), vv)):
            swapped = pltpu.roll(cells, HEAD, 1)
            dst[0, at, :] = jnp.where(low, cells, swapped).astype(BF)
            dst[1, at, :] = jnp.where(low, swapped, cells).astype(BF)
        return carry

    @pl.when(s == 0)
    def _():
        kv[pl.ds(0, WINDOW), :] = jnp.zeros((WINDOW, kv.shape[1]), BF)

    @pl.when(s == last)
    def _():
        kv[pl.ds(tokens + WINDOW, WINDOW), :] = jnp.zeros((WINDOW, kv.shape[1]), BF)

    whole_k.wait()
    whole_v.wait()
    lax.fori_loop(1, blocks + 1, spread, 0)
    for after, before in halos:
        pl.when(s > 0)(after.wait_recv)
        pl.when(s < last)(before.wait_recv)
    spread(0, 0)
    spread(blocks + 1, 0)
    whole_q.wait()

    heads = qv.shape[1] // HEAD
    kv_count = kk.shape[0]
    group = heads // kv_count
    firsts = (blocks + 1) // 2

    def attend(i, carry):
        n = jnp.where(i < firsts, blocks - firsts + i, blocks - 1 - i)
        n = jnp.where(y == 0, n, blocks - 1 - n)
        base = pl.multiple_of(n * WINDOW, WINDOW)
        shape = (WINDOW, 3 * WINDOW)
        q_at = lax.broadcasted_iota(jnp.int32, shape, 0)
        k_at = lax.broadcasted_iota(jnp.int32, shape, 1) - WINDOW
        place = k_at + (s * tokens + base)
        valid = (jnp.abs(k_at - q_at) <= WINDOW) & (place >= 0) & (place < total)
        cosine, sine = angles(n + 1)
        for g in range(kv_count):
            qs = []
            for j in range(group // 2):
                at = (g * group // 2 + j) * LANES
                two = turned(qv[pl.ds(base, WINDOW), at : at + LANES], cosine, sine).astype(BF) * BF(HEAD ** -0.5)
                qs += [jnp.where(low, two, BF(0)), jnp.where(low, BF(0), two)]
            k = kk[g, pl.ds(base, 3 * WINDOW), :]
            v = vv[g, pl.ds(base, 3 * WINDOW), :]
            scores = lax.dot_general(jnp.concatenate(qs, 0), k, (((1,), (1,)), ((), ())), preferred_element_type=F32)
            parts, shares = [], []
            for j in range(group):
                sc = jnp.where(valid, scores[j * WINDOW : (j + 1) * WINDOW], -jnp.inf)
                sink = sink_ref[g * group + j]
                top = jnp.maximum(jnp.max(sc, -1, keepdims=True), sink)
                raised = jnp.exp(sc - top)
                denom = jnp.sum(raised, -1, keepdims=True) + jnp.exp(sink - top)
                parts.append(raised.astype(BF))
                shares.append(1.0 / denom)
            outs = jnp.dot(jnp.concatenate(parts, 0), v, preferred_element_type=F32)
            outs = [outs[j * WINDOW : (j + 1) * WINDOW] * shares[j] for j in range(group)]
            for j in range(group // 2):
                at = (g * group // 2 + j) * LANES
                att[pl.ds(base, WINDOW), at : at + LANES] = jnp.where(low, outs[2 * j], outs[2 * j + 1]).astype(BF)
        return carry

    step = 4 * LANES
    wide = model // 2

    def project(which):
        begin = pl.multiple_of((y if which else 1 - y) * 2 * rows, 32)
        for m in range(2):
            def body(n, carry):
                cols = pl.ds(pl.multiple_of(m * wide + n * step, step), step)
                both = jnp.dot(att[pl.ds(begin, 2 * rows), :], wv[:, cols], preferred_element_type=F32)
                kept[which, :, :, cols] = both.reshape(2, rows, step)
                p_send[which, :, cols] = kept[which, 1 - c, :, cols].astype(BF)
                return carry

            lax.fori_loop(0, wide // step, body, 0)
            by_core(which, m).start()

    def by_core(which, m):
        cols = pl.ds(m * wide, wide)
        return send(p_send.at[which, :, cols], p_recv.at[which, :, cols], p_ss.at[which, m], p_rs.at[which, m], at_c)

    def by_y(m):
        cols = pl.ds(m * wide, wide)
        return send(y_send.at[:, cols], y_recv.at[:, cols], p_ss.at[2, m], p_rs.at[2, m], at_y)

    lax.fori_loop(0, firsts, attend, 0)
    whole_w.wait()
    project(0)
    lax.fori_loop(firsts, firsts + 1, attend, 0)
    for m in range(2):
        by_core(0, m).wait_recv()
        cols = slice(m * wide, (m + 1) * wide)
        y_send[:, cols] = (kept[0, c, :, cols] + p_recv[0, :, cols].astype(F32)).astype(BF)
        by_y(m).start()
    lax.fori_loop(firsts + 1, blocks, attend, 0)
    project(1)
    whole_s.wait()
    relay(0, "n")
    relay(1, "s")
    for m in range(2):
        by_core(1, m).wait_recv()
        by_y(m).wait_recv()
        cols = slice(m * wide, (m + 1) * wide)
        mix = kept[1, c, :, cols] + p_recv[1, :, cols].astype(F32) + y_recv[:, cols].astype(F32)
        mixed[:, cols] = (sv[:, cols].astype(F32) + mix).astype(BF)
    whole = mixed[...].astype(F32)
    scale = lax.rsqrt(jnp.mean(whole * whole, -1, keepdims=True) + 1e-06)
    nt[0, 0] = (whole * scale * gain_ref[...]).astype(BF)

    to_n = send(nt.at[0, 0], nt.at[0, 1], n_ss.at[0], n_rs.at[0], at_n)
    to_y = send(nt.at[0, 0], nt.at[0, 2], n_ss.at[1], n_rs.at[1], at_y)
    on_y = send(nt.at[0, 1], nt.at[0, 3], n_ss.at[2], n_rs.at[2], at_y)
    to_c = [send(nt.at[0, g], nt.at[1, g], n_ss.at[3 + g], n_rs.at[3 + g], at_c) for g in range(4)]
    to_n.start()
    to_y.start()
    to_c[0].start()
    pl.when(outer)(lambda: push(0, "f"))
    relay(1, "n")
    to_n.wait_recv()
    on_y.start()
    to_c[1].start()
    relay(0, "o")
    to_y.wait_recv()
    to_c[2].start()
    relay(0, "f", range(2))
    on_y.wait_recv()
    to_c[3].start()
    relay(0, "f", range(2, GCH))
    push(1, "o")
    push(1, "f")
    for copy in to_c:
        copy.wait_recv()
    for name in NAMES:
        crossed(0, name)

    depth = gu.shape[0] * gu.shape[1]

    def units(q, cols, size):
        both = jnp.dot(nt[q].reshape(4 * rows, model), gu[:, :, cols].reshape(depth, size), preferred_element_type=F32)
        gate = both[:, : size // 2]
        return (gate / (1.0 + jnp.exp(-gate)) * both[:, size // 2 :]).astype(BF)

    def hidden_of(q):
        def body(n, carry):
            cols = pl.ds(pl.multiple_of(n * 2 * LANES, 2 * LANES), 2 * LANES)
            hid[q, :, pl.ds(pl.multiple_of(n * LANES, LANES), LANES)] = units(q, cols, 2 * LANES)
            return carry

        lax.fori_loop(0, per, body, 0)
        hid[q, :, cut:] = units(q, pl.ds(edge, 2 * tail), 2 * tail)

    hidden_of(0)
    relay(1, "o")
    hidden_of(1)
    relay(1, "f")

    wide_d = dn.shape[2]
    order = [("s", 0), ("s", 1), ("n", 0), ("n", 1), ("o", 0), ("f", 0), ("o", 1), ("f", 1)]

    def slot_at(i):
        name, side = order[i]
        return 2 * dests[name] + (x if side == 0 else 1 - x)

    twin = [order.index(({"s": "n", "n": "s", "o": "f", "f": "o"}[name], side)) for name, side in order]

    def exchange(which, i):
        src, dst = ((c_send, c_recv), (s1, r1), (s2, r2))[which]
        on_z = which and (which == 1) == (order[i][1] == 1)
        there = twin[i] if on_z else i
        to = at_n if on_z else (at_y if which else at_c)
        return send(src.at[i], dst.at[there], e_ss.at[which, i], e_rs.at[which, there], to)

    def arrived(which, i):
        on_z = which and (which == 1) == (order[i][1] == 1)
        exchange(which, twin[i] if on_z else i).wait_recv()

    def lower(i):
        name, side = order[i]
        if side:
            crossed(1, name)
        slot = slot_at(i)
        c_send[i] = jnp.dot(hid[1], dn[slot], preferred_element_type=F32).astype(BF)
        exchange(0, i).start()
        acc[i] = jnp.dot(hid[0], dn[slot], preferred_element_type=F32).reshape(4, rows, wide_d)

    def first(i):
        arrived(0, i)
        both = acc[i] + c_recv[i].reshape(4, rows, wide_d).astype(F32)
        away = (1, 3) if order[i][1] else (2, 3)
        for j in range(2):
            s1[i, j] = both[away[j]].astype(BF)
        exchange(1, i).start()
        acc[i, 0] = both[0]
        acc[i, 1] = both[2 if order[i][1] else 1]

    def second(i):
        arrived(1, i)
        s2[i] = (acc[i, 1] + r1[i, 1].astype(F32)).astype(BF)
        exchange(2, i).start()

    def finish(i):
        arrived(2, i)
        cols = pl.ds(pl.multiple_of(slot_at(i) * wide_d, wide_d), wide_d)
        lowered = acc[i, 0] + r1[i, 0].astype(F32) + r2[i].astype(F32)
        out_ref[:, cols] = (mixed[:, cols].astype(F32) + 0.5 * lowered).astype(BF)

    count = len(order)
    for i in range(count + 1):
        if i < count:
            lower(i)
        if i > 0:
            first(i - 1)
        if i > 3:
            second(i - 4)
    for i in range(count - 3, count):
        second(i)
        if i < count - 1:
            finish(2 * (i - count + 3))
            finish(2 * (i - count + 3) + 1)
    for i in range(4, count):
        finish(i)

    for after, before in halos:
        pl.when(s < last)(after.wait_send)
        pl.when(s > 0)(before.wait_send)
    for kind in range(2):
        for name in NAMES:
            for g in range(chunks[kind]):
                by_x(kind, name, g).wait_send()
                if name != "s":
                    by_z(kind, name, g).wait_send()
    for m in range(2):
        for copy in (by_core(0, m), by_core(1, m), by_y(m)):
            copy.wait_send()
    for copy in [to_n, to_y, on_y] + to_c:
        copy.wait_send()
    for which in range(3):
        for i in range(len(order)):
            exchange(which, i).wait_send()


def local_lines(
    queries, keys, values, sink, stream, out_weight, norm_gain, gate_weight, up_weight, down_weight
):
    length = lax.axis_size("sp") // 2
    tokens = queries.shape[0]
    rows, model = stream.shape
    depth, wide = gate_weight.shape
    per = wide // LANES // 2
    tail = wide // 2 - per * LANES
    half = wide // 2
    slots = 2 * length
    part = down_weight.shape[1]
    blocks = tokens // WINDOW
    within, begins = turn_tables(slots * blocks + 2)
    vmem = pl.BlockSpec(memory_space=pltpu.VMEM)
    far = pl.BlockSpec(memory_space=pl.ANY)
    dma = pltpu.SemaphoreType.DMA
    dims = (length, tokens, rows, per, tail, tokens * slots)
    return pl.pallas_call(
        functools.partial(layer_kernel, dims),
        out_shape=jax.ShapeDtypeStruct((rows, model), BF),
        in_specs=[far] * 3 + [pl.BlockSpec(memory_space=pltpu.SMEM)] + [far] * 2 + [vmem] + [far] * 3 + [vmem] * 2,
        out_specs=vmem,
        scratch_shapes=[
            pltpu.VMEM(queries.shape, BF),
            pltpu.VMEM((tokens + 2 * WINDOW, 2 * LANES), BF),
            pltpu.VMEM((2, tokens + 2 * WINDOW, LANES), BF),
            pltpu.VMEM((2, tokens + 2 * WINDOW, LANES), BF),
            pltpu.VMEM(queries.shape, BF),
            pltpu.VMEM(out_weight.shape, BF),
            pltpu.VMEM(stream.shape, BF),
            pltpu.VMEM((2, depth, LANES), BF),
            pltpu.VMEM((depth, wide), BF),
            pltpu.VMEM((half, part), BF),
            pltpu.VMEM((slots, depth, wide), BF),
            pltpu.VMEM((slots, half, part), BF),
            pltpu.VMEM((2, rows, model), BF),
            pltpu.VMEM((2, rows, model), BF),
            pltpu.VMEM((2, 2, rows, model), F32),
            pltpu.VMEM((rows, model), BF),
            pltpu.VMEM((rows, model), BF),
            pltpu.VMEM((rows, model), BF),
            pltpu.VMEM((2, 4, rows, model), BF),
            pltpu.VMEM((2, 4 * rows, half), BF),
            pltpu.VMEM((slots, 4 * rows, part), BF),
            pltpu.VMEM((slots, 4 * rows, part), BF),
            pltpu.VMEM((slots, 4, rows, part), F32),
            pltpu.VMEM((slots, 2, rows, part), BF),
            pltpu.VMEM((slots, 2, rows, part), BF),
            pltpu.VMEM((slots, rows, part), BF),
            pltpu.VMEM((slots, rows, part), BF),
            dma((10,)), dma((2, 2)), dma((2, 2)),
            dma((2, 3, GCH)), dma((2, 4, GCH)), dma((slots, GCH)), dma((slots, DCH)),
            dma((3, 2)), dma((3, 2)), dma((7,)), dma((7,)), dma((3, slots)), dma((3, slots)),
        ],
        compiler_params=pltpu.CompilerParams(
            collective_id=0, has_side_effects=True, vmem_limit_bytes=63 * 1024 * 1024
        ),
    )(
        queries, keys, values, sink, stream, out_weight, norm_gain[None],
        gate_weight, up_weight, down_weight, jnp.asarray(within), jnp.asarray(begins),
    )


def solution(mesh):
    placed = (
        P("sp", "tp"),
        P("sp", "tp"),
        P("sp", "tp"),
        P("tp"),
        P(("sp", "tp"), None),
        P("tp", None),
        P(),
        P("sp", "tp"),
        P("sp", "tp"),
        P("tp", "sp"),
    )
    lines = mesh.shape["tp"] == 4 and mesh.shape["sp"] == 8
    return jax.shard_map(
        local_lines if lines else local, mesh=mesh, in_specs=placed, out_specs=P(("sp", "tp"), None), check_vma=False
    )
```

```python
import functools

import jax
import jax.numpy as jnp
import numpy as np
from jax import lax
from jax.experimental import pallas as pl
from jax.experimental.pallas import tpu as pltpu
from jax.sharding import PartitionSpec as P

HEAD = 64
WINDOW = 128
LANES = 128
BF = jnp.bfloat16
F32 = jnp.float32
MESH = pl.DeviceIdType.MESH


def padded_2(cells, sides, width):
    for axis, dim in sides:
        count = lax.axis_size(axis)
        ends = count - 1
        head = lax.slice_in_dim(cells, 0, width, axis=dim)
        tail = lax.slice_in_dim(cells, cells.shape[dim] - width, cells.shape[dim], axis=dim)
        cells = jnp.concatenate(
            [
                lax.ppermute(tail, axis, [(i, (i + 1) % count) for i in range(ends)]),
                cells,
                lax.ppermute(head, axis, [((i + 1) % count, i) for i in range(ends)]),
            ],
            axis=dim,
        )
    return cells


def rotary(block, start):
    length = block.shape[0]
    middle = HEAD // 2
    inverse = 1.0 / 10000.0 ** (jnp.arange(0, HEAD, 2, dtype=jnp.float32) / HEAD)
    places = (start + jnp.arange(length, dtype=jnp.int32)).astype(jnp.float32)
    angles = places[:, None, None] * inverse[None, None, :]
    cosine_table = jnp.cos(angles)
    sine_table = jnp.sin(angles)
    pieces = block.astype(jnp.float32).reshape(length, -1, HEAD)
    leading = pieces[..., :middle]
    trailing = pieces[..., middle:]
    turned = jnp.concatenate(
        [
            leading * cosine_table - trailing * sine_table,
            trailing * cosine_table + leading * sine_table,
        ],
        -1,
    )
    return turned.reshape(length, -1).astype(jnp.bfloat16)


def window_attend(queries, keys, values, sink):
    rows_here = queries.shape[0]
    start = lax.axis_index("sp") * rows_here
    length = lax.axis_size("sp") * rows_here
    blocks = rows_here // WINDOW
    kv_width = keys.shape[1]
    kv_count = kv_width // HEAD
    head_count = queries.shape[1] // HEAD
    group = head_count // kv_count
    turned_q = rotary(queries, start)
    turned_k = rotary(keys, start)
    paired = jnp.concatenate([turned_k, values], 1)
    padded = padded_2(paired, (("sp", 0),), WINDOW)
    framed = padded.reshape(blocks + 2, WINDOW, 2 * kv_width)
    banded = jnp.concatenate([framed[:-2], framed[1:-1], framed[2:]], axis=1)
    key_band = banded[..., :kv_width].reshape(blocks, 3 * WINDOW, kv_count, HEAD)
    value_band = banded[..., kv_width:].reshape(blocks, 3 * WINDOW, kv_count, HEAD)
    query_blocks = turned_q.reshape(blocks, WINDOW, kv_count, group, HEAD)
    scores = jnp.einsum(
        "nqkgd,nskd->nkgqs", query_blocks, key_band, preferred_element_type=jnp.float32
    ) * HEAD ** (-0.5)
    query_place = (
        start + jnp.arange(blocks)[:, None, None] * WINDOW + jnp.arange(WINDOW)[None, :, None]
    )
    key_place = (
        start
        + jnp.arange(blocks)[:, None, None] * WINDOW
        - WINDOW
        + jnp.arange(3 * WINDOW)[None, None, :]
    )
    valid = (jnp.abs(key_place - query_place) <= WINDOW) & (key_place >= 0) & (key_place < length)
    scores = jnp.where(valid[:, None, None], scores, -jnp.inf)
    sink_grid = sink.reshape(kv_count, group)[None, :, :, None]
    top = jnp.maximum(jnp.max(scores, -1), sink_grid)
    raised = jnp.exp(scores - top[..., None])
    denom = jnp.sum(raised, -1) + jnp.exp(sink_grid - top)
    weights = (raised / denom[..., None]).astype(jnp.bfloat16)
    output = jnp.einsum(
        "nkgqs,nskd->nqkgd", weights, value_band, preferred_element_type=jnp.float32
    )
    return output.astype(jnp.bfloat16).reshape(rows_here, head_count * HEAD)


def collect_weights(gate_weight, up_weight, down_weight):
    return (
        lax.all_gather(gate_weight, "sp", axis=0, tiled=True),
        lax.all_gather(up_weight, "sp", axis=0, tiled=True),
        lax.all_gather(down_weight, "sp", axis=1, tiled=True),
    )


def local(
    queries, keys, values, sink, stream, out_weight, norm_gain, gate_weight, up_weight, down_weight
):
    attended = window_attend(queries, keys, values, sink)
    gathered = collect_weights(gate_weight, up_weight, down_weight)
    gate_whole, up_whole, down_whole = gathered
    rows = attended
    projected = lax.psum_scatter(
        jnp.dot(rows, out_weight, preferred_element_type=jnp.float32),
        "tp",
        scatter_dimension=0,
        tiled=True,
    )
    mixed = (stream.astype(jnp.float32) + projected).astype(jnp.bfloat16)
    mixed_wide = mixed.astype(jnp.float32)
    scale = lax.rsqrt(jnp.mean(mixed_wide * mixed_wide, -1, keepdims=True) + 1e-06)
    normed = (mixed_wide * scale * norm_gain).astype(jnp.bfloat16)
    piece = lax.all_gather(normed, "tp", axis=0, tiled=True)
    gate = jnp.dot(piece, gate_whole, preferred_element_type=jnp.float32)
    upward = jnp.dot(piece, up_whole, preferred_element_type=jnp.float32)
    hidden = (jax.nn.silu(gate) * upward).astype(jnp.bfloat16)
    rows = hidden
    lowered = lax.psum_scatter(
        jnp.dot(rows, down_whole, preferred_element_type=jnp.float32).astype(jnp.bfloat16),
        "tp",
        scatter_dimension=0,
        tiled=True,
    ).astype(jnp.float32)
    return (mixed_wide + 0.5 * lowered).astype(jnp.bfloat16)


def turn_tables(blocks):
    lane = np.arange(LANES)
    inverse = 10000.0 ** (-2.0 * (lane % (HEAD // 2)) / HEAD)
    within = np.arange(WINDOW)[:, None] * inverse[None, :]
    begins = (np.arange(blocks) - 1)[:, None] * WINDOW * inverse[None, :]
    pair = lambda a: np.stack([np.cos(a), np.sin(a)]).astype(np.float32)
    return pair(within), pair(begins)


NAMES = "onfs"
GCH, DCH = 4, 4


def layer_kernel(
    dims, q_in, k_in, v_in, sink_ref, stream_in, w_in, gain_ref, gate_in, up_in, down_in, turn_ref, begin_ref,
    out_ref,
    qv, kv, kk, vv, att, wv, sv, tails, oth, doth, gu, dn, p_send, p_recv, kept, y_send, y_recv, mixed, nt,
    hid, c_send, c_recv, acc, s1, r1, s2, r2,
    loc, h_ss, h_rs, z_ss, x_ss, gu_rs, d_rs, p_ss, p_rs, n_ss, n_rs, e_ss, e_rs,
):
    length, tokens, rows, per, tail, total = dims
    s = lax.axis_index("sp")
    z, x = s // 2, s % 2
    t = lax.axis_index("tp")
    y, c = t // 2, t % 2
    part = z % 2
    pz = z + 1 - 2 * part
    half = length // 2
    flip = lambda q: q + half - 2 * half * (q // half)
    fz, fp = flip(z), flip(pz)
    dests = {"o": fz, "n": pz, "f": fp, "s": z}
    outer = (z == 0) | (z == length - 1)
    at_x = {"sp": s + 1 - 2 * x}
    at_n = {"sp": 2 * pz + x}
    at_y = {"tp": t + 2 - 4 * y}
    at_c = {"tp": t + 1 - 2 * c}
    last = 2 * length - 1
    model = out_ref.shape[1]
    blocks = tokens // WINDOW
    edge = per * 2 * LANES
    cut = per * LANES

    def send(src, dst, ssem, rsem, to):
        return pltpu.make_async_remote_copy(
            src_ref=src, dst_ref=dst, send_sem=ssem, recv_sem=rsem,
            device_id=to, device_id_type=MESH,
        )

    def fetch(src, dst, i):
        return pltpu.make_async_copy(src, dst, loc.at[i])

    def fetch_part(which, dst, i):
        for n in range(per):
            at = pl.multiple_of((which * per + n) * LANES, LANES)
            for side, src in ((0, gate_in), (1, up_in)):
                fetch(src.at[:, pl.ds(at, LANES)], dst.at[:, pl.ds((2 * n + side) * LANES, LANES)], i).start()

    def fetch_down(which, dst, i):
        fetch(down_in.at[pl.ds(pl.multiple_of(which * cut, LANES), cut)], dst.at[pl.ds(0, cut)], i).start()
        at = pl.multiple_of(edge + which * tail, tail)
        fetch(down_in.at[pl.ds(at, tail)], dst.at[pl.ds(cut, tail)], i).start()

    whole_k = fetch(k_in, kv.at[pl.ds(WINDOW, tokens), pl.ds(0, LANES)], 3)
    whole_v = fetch(v_in, kv.at[pl.ds(WINDOW, tokens), pl.ds(LANES, LANES)], 4)
    whole_q = fetch(q_in, qv, 5)
    whole_w = fetch(w_in, wv, 8)
    whole_s = fetch(stream_in, sv, 9)
    fetch_part(1 - part, oth, 0)
    fetch(gate_in.at[:, pl.ds(edge, LANES)], tails.at[0], 2).start()
    fetch(up_in.at[:, pl.ds(edge, LANES)], tails.at[1], 2).start()
    fetch_part(part, gu.at[s], 1)
    whole_k.start()
    whole_v.start()
    fetch_down(1 - part, doth, 7)
    whole_q.start()
    fetch_down(part, dn.at[s], 6)
    whole_w.start()
    whole_s.start()

    barrier = pltpu.get_barrier_semaphore()

    def greet(to):
        pl.semaphore_signal(barrier, inc=1, device_id=to, device_id_type=MESH)

    for to in (at_x, at_n, {"sp": 2 * fz + x}, {"sp": 2 * fp + x}, at_y, at_c):
        greet(to)
    hop_up = (x == 1) & (z < length - 1)
    hop_down = (x == 0) & (z > 0)
    pl.when(hop_up)(lambda: greet({"sp": s + 1}))
    pl.when(hop_down)(lambda: greet({"sp": s - 1}))
    pl.semaphore_wait(barrier, 6 + hop_up.astype(jnp.int32) + hop_down.astype(jnp.int32))

    halos = []
    for i, src in ((0, k_in), (1, v_in)):
        cols = pl.ds(i * LANES, LANES)
        after = send(src.at[pl.ds(tokens - WINDOW, WINDOW)], kv.at[pl.ds(0, WINDOW), cols], h_ss.at[0, i], h_rs.at[0, i], {"sp": s + 1})
        before = send(src.at[pl.ds(0, WINDOW)], kv.at[pl.ds(tokens + WINDOW, WINDOW), cols], h_ss.at[1, i], h_rs.at[1, i], {"sp": s - 1})
        pl.when(s < last)(after.start)
        pl.when(s > 0)(before.start)
        halos.append((after, before))

    chunks = (GCH, DCH)

    def piece(kind, ref, g):
        size = (gu, dn)[kind].shape[1] // chunks[kind]
        return ref.at[pl.ds(g * size, size)]

    def slot_of(name):
        return 2 * dests[name] + x

    def buffers(kind):
        return ((gu, gu_rs), (dn, d_rs))[kind]

    def by_z(kind, name, g):
        buf, got = buffers(kind)
        src = buf.at[s] if name == "o" else (oth, doth)[kind]
        sem = z_ss.at[kind, NAMES.index(name), g]
        return send(piece(kind, src, g), piece(kind, buf.at[s], g), sem, got.at[s, g], {"sp": slot_of(name)})

    def by_x(kind, name, g):
        buf, got = buffers(kind)
        here = piece(kind, buf.at[slot_of(name)], g)
        return send(here, here, x_ss.at[kind, NAMES.index(name), g], got.at[slot_of(name), g], at_x)

    def landed(kind, slot, g):
        buf, got = buffers(kind)
        here = piece(kind, buf.at[slot], g)
        send(here, here, x_ss.at[0, 0, 0], got.at[slot, g], at_x).wait_recv()

    def push(kind, name):
        for g in range(chunks[kind]):
            by_z(kind, name, g).start()

    def relay(kind, name, some=None):
        for g in range(chunks[kind]) if some is None else some:
            if name != "s":
                landed(kind, slot_of(name), g)
            by_x(kind, name, g).start()

    def crossed(kind, name):
        for g in range(chunks[kind]):
            landed(kind, 2 * dests[name] + 1 - x, g)

    fetch(oth.at[:, pl.ds(0, edge)], oth.at[:, pl.ds(0, edge)], 0).wait()
    fetch(tails, tails, 2).wait()
    low_tail = jnp.concatenate([tails[0, :, :tail], tails[1, :, :tail]], 1)
    high_tail = jnp.concatenate([tails[0, :, tail:], tails[1, :, tail:]], 1)
    oth[:, edge:] = jnp.where(part == 0, high_tail, low_tail)
    gu[s, :, edge:] = jnp.where(part == 0, low_tail, high_tail)
    push(0, "n")
    own = gu.at[s, :, pl.ds(0, edge)]
    fetch(own, own, 1).wait()
    relay(0, "s")
    fetch(doth, doth, 7).wait()
    push(1, "n")
    push(0, "o")
    pl.when(jnp.logical_not(outer))(lambda: push(0, "f"))
    fetch(dn.at[s], dn.at[s], 6).wait()

    lane = lax.broadcasted_iota(jnp.int32, (WINDOW, LANES), 1)
    low = lane < HEAD
    front = lane % HEAD < HEAD // 2

    def angles(m):
        row = s * blocks + m
        cos_b, sin_b = begin_ref[0, pl.ds(row, 1), :], begin_ref[1, pl.ds(row, 1), :]
        cosine = turn_ref[0] * cos_b - turn_ref[1] * sin_b
        sine = turn_ref[1] * cos_b + turn_ref[0] * sin_b
        return cosine, jnp.where(front, -sine, sine)

    def turned(block, cosine, sine):
        cells = block.astype(F32)
        other = jnp.where(front, pltpu.roll(cells, LANES - HEAD // 2, 1), pltpu.roll(cells, HEAD // 2, 1))
        return cells * cosine + other * sine

    def spread(m, carry):
        at = pl.ds(pl.multiple_of(m * WINDOW, WINDOW), WINDOW)
        cosine, sine = angles(m)
        for cells, dst in ((turned(kv[at, :LANES], cosine, sine), kk), (kv[at, LANES:].astype(F32), vv)):
            swapped = pltpu.roll(cells, HEAD, 1)
            dst[0, at, :] = jnp.where(low, cells, swapped).astype(BF)
            dst[1, at, :] = jnp.where(low, swapped, cells).astype(BF)
        return carry

    @pl.when(s == 0)
    def _():
        kv[pl.ds(0, WINDOW), :] = jnp.zeros((WINDOW, kv.shape[1]), BF)

    @pl.when(s == last)
    def _():
        kv[pl.ds(tokens + WINDOW, WINDOW), :] = jnp.zeros((WINDOW, kv.shape[1]), BF)

    whole_k.wait()
    whole_v.wait()
    lax.fori_loop(1, blocks + 1, spread, 0)
    for after, before in halos:
        pl.when(s > 0)(after.wait_recv)
        pl.when(s < last)(before.wait_recv)
    spread(0, 0)
    spread(blocks + 1, 0)
    whole_q.wait()

    heads = qv.shape[1] // HEAD
    kv_count = kk.shape[0]
    group = heads // kv_count
    firsts = (blocks + 1) // 2

    def attend(i, carry):
        n = jnp.where(i < firsts, blocks - firsts + i, blocks - 1 - i)
        n = jnp.where(y == 0, n, blocks - 1 - n)
        base = pl.multiple_of(n * WINDOW, WINDOW)
        shape = (WINDOW, 3 * WINDOW)
        q_at = lax.broadcasted_iota(jnp.int32, shape, 0)
        k_at = lax.broadcasted_iota(jnp.int32, shape, 1) - WINDOW
        place = k_at + (s * tokens + base)
        valid = (jnp.abs(k_at - q_at) <= WINDOW) & (place >= 0) & (place < total)
        cosine, sine = angles(n + 1)
        for g in range(kv_count):
            qs = []
            for j in range(group // 2):
                at = (g * group // 2 + j) * LANES
                two = turned(qv[pl.ds(base, WINDOW), at : at + LANES], cosine, sine).astype(BF) * BF(HEAD ** -0.5)
                qs += [jnp.where(low, two, BF(0)), jnp.where(low, BF(0), two)]
            k = kk[g, pl.ds(base, 3 * WINDOW), :]
            v = vv[g, pl.ds(base, 3 * WINDOW), :]
            scores = lax.dot_general(jnp.concatenate(qs, 0), k, (((1,), (1,)), ((), ())), preferred_element_type=F32)
            parts, shares = [], []
            for j in range(group):
                sc = jnp.where(valid, scores[j * WINDOW : (j + 1) * WINDOW], -jnp.inf)
                sink = sink_ref[g * group + j]
                top = jnp.maximum(jnp.max(sc, -1, keepdims=True), sink)
                raised = jnp.exp(sc - top)
                denom = jnp.sum(raised, -1, keepdims=True) + jnp.exp(sink - top)
                parts.append(raised.astype(BF))
                shares.append(1.0 / denom)
            outs = jnp.dot(jnp.concatenate(parts, 0), v, preferred_element_type=F32)
            outs = [outs[j * WINDOW : (j + 1) * WINDOW] * shares[j] for j in range(group)]
            for j in range(group // 2):
                at = (g * group // 2 + j) * LANES
                att[pl.ds(base, WINDOW), at : at + LANES] = jnp.where(low, outs[2 * j], outs[2 * j + 1]).astype(BF)
        return carry

    step = 4 * LANES
    wide = model // 2

    def project(which):
        begin = pl.multiple_of((y if which else 1 - y) * 2 * rows, 32)
        for m in range(2):
            def body(n, carry):
                cols = pl.ds(pl.multiple_of(m * wide + n * step, step), step)
                both = jnp.dot(att[pl.ds(begin, 2 * rows), :], wv[:, cols], preferred_element_type=F32)
                kept[which, :, :, cols] = both.reshape(2, rows, step)
                p_send[which, :, cols] = kept[which, 1 - c, :, cols].astype(BF)
                return carry

            lax.fori_loop(0, wide // step, body, 0)
            by_core(which, m).start()

    def by_core(which, m):
        cols = pl.ds(m * wide, wide)
        return send(p_send.at[which, :, cols], p_recv.at[which, :, cols], p_ss.at[which, m], p_rs.at[which, m], at_c)

    def by_y(m):
        cols = pl.ds(m * wide, wide)
        return send(y_send.at[:, cols], y_recv.at[:, cols], p_ss.at[2, m], p_rs.at[2, m], at_y)

    lax.fori_loop(0, firsts, attend, 0)
    whole_w.wait()
    project(0)
    lax.fori_loop(firsts, firsts + 1, attend, 0)
    for m in range(2):
        by_core(0, m).wait_recv()
        cols = slice(m * wide, (m + 1) * wide)
        y_send[:, cols] = (kept[0, c, :, cols] + p_recv[0, :, cols].astype(F32)).astype(BF)
        by_y(m).start()
    lax.fori_loop(firsts + 1, blocks, attend, 0)
    project(1)
    whole_s.wait()
    relay(0, "n")
    relay(1, "s")
    for m in range(2):
        by_core(1, m).wait_recv()
        by_y(m).wait_recv()
        cols = slice(m * wide, (m + 1) * wide)
        mix = kept[1, c, :, cols] + p_recv[1, :, cols].astype(F32) + y_recv[:, cols].astype(F32)
        mixed[:, cols] = (sv[:, cols].astype(F32) + mix).astype(BF)
    whole = mixed[...].astype(F32)
    scale = lax.rsqrt(jnp.mean(whole * whole, -1, keepdims=True) + 1e-06)
    nt[0, 0] = (whole * scale * gain_ref[...]).astype(BF)

    to_n = send(nt.at[0, 0], nt.at[0, 1], n_ss.at[0], n_rs.at[0], at_n)
    to_y = send(nt.at[0, 0], nt.at[0, 2], n_ss.at[1], n_rs.at[1], at_y)
    on_y = send(nt.at[0, 1], nt.at[0, 3], n_ss.at[2], n_rs.at[2], at_y)
    to_c = [send(nt.at[0, g], nt.at[1, g], n_ss.at[3 + g], n_rs.at[3 + g], at_c) for g in range(4)]
    to_n.start()
    to_y.start()
    to_c[0].start()
    pl.when(outer)(lambda: push(0, "f"))
    relay(1, "n")
    to_n.wait_recv()
    on_y.start()
    to_c[1].start()
    relay(0, "o")
    to_y.wait_recv()
    to_c[2].start()
    relay(0, "f", range(2))
    push(1, "o")
    push(1, "f")
    on_y.wait_recv()
    to_c[3].start()
    relay(0, "f", range(2, GCH))
    for copy in to_c:
        copy.wait_recv()
    for name in NAMES:
        crossed(0, name)

    depth = gu.shape[0] * gu.shape[1]

    def units(q, cols, size):
        both = jnp.dot(nt[q].reshape(4 * rows, model), gu[:, :, cols].reshape(depth, size), preferred_element_type=F32)
        gate = both[:, : size // 2]
        return (gate / (1.0 + jnp.exp(-gate)) * both[:, size // 2 :]).astype(BF)

    def hidden_of(q):
        def body(n, carry):
            cols = pl.ds(pl.multiple_of(n * 2 * LANES, 2 * LANES), 2 * LANES)
            hid[q, :, pl.ds(pl.multiple_of(n * LANES, LANES), LANES)] = units(q, cols, 2 * LANES)
            return carry

        lax.fori_loop(0, per, body, 0)
        hid[q, :, cut:] = units(q, pl.ds(edge, 2 * tail), 2 * tail)

    hidden_of(0)
    relay(1, "o")
    hidden_of(1)
    relay(1, "f")

    wide_d = dn.shape[2]
    order = [("s", 0), ("s", 1), ("n", 0), ("n", 1), ("o", 0), ("f", 0), ("o", 1), ("f", 1)]

    def slot_at(i):
        name, side = order[i]
        return 2 * dests[name] + (x if side == 0 else 1 - x)

    twin = [order.index(({"s": "n", "n": "s", "o": "f", "f": "o"}[name], side)) for name, side in order]

    def exchange(which, i):
        src, dst = ((c_send, c_recv), (s1, r1), (s2, r2))[which]
        on_z = which and (which == 1) == (order[i][1] == 1)
        there = twin[i] if on_z else i
        to = at_n if on_z else (at_y if which else at_c)
        return send(src.at[i], dst.at[there], e_ss.at[which, i], e_rs.at[which, there], to)

    def arrived(which, i):
        on_z = which and (which == 1) == (order[i][1] == 1)
        exchange(which, twin[i] if on_z else i).wait_recv()

    def lower(i):
        name, side = order[i]
        if side:
            crossed(1, name)
        slot = slot_at(i)
        c_send[i] = jnp.dot(hid[1], dn[slot], preferred_element_type=F32).astype(BF)
        exchange(0, i).start()
        acc[i] = jnp.dot(hid[0], dn[slot], preferred_element_type=F32).reshape(4, rows, wide_d)

    def first(i):
        arrived(0, i)
        both = acc[i] + c_recv[i].reshape(4, rows, wide_d).astype(F32)
        away = (1, 3) if order[i][1] else (2, 3)
        for j in range(2):
            s1[i, j] = both[away[j]].astype(BF)
        exchange(1, i).start()
        acc[i, 0] = both[0]
        acc[i, 1] = both[2 if order[i][1] else 1]

    def second(i):
        arrived(1, i)
        s2[i] = (acc[i, 1] + r1[i, 1].astype(F32)).astype(BF)
        exchange(2, i).start()

    def finish(i):
        arrived(2, i)
        cols = pl.ds(pl.multiple_of(slot_at(i) * wide_d, wide_d), wide_d)
        lowered = acc[i, 0] + r1[i, 0].astype(F32) + r2[i].astype(F32)
        out_ref[:, cols] = (mixed[:, cols].astype(F32) + 0.5 * lowered).astype(BF)

    count = len(order)
    for i in range(count + 1):
        if i < count:
            lower(i)
        if i > 0:
            first(i - 1)
        if i > 3:
            second(i - 4)
    for i in range(count - 3, count):
        second(i)
        if i < count - 1:
            finish(2 * (i - count + 3))
            finish(2 * (i - count + 3) + 1)
    for i in range(4, count):
        finish(i)

    for after, before in halos:
        pl.when(s < last)(after.wait_send)
        pl.when(s > 0)(before.wait_send)
    for kind in range(2):
        for name in NAMES:
            for g in range(chunks[kind]):
                by_x(kind, name, g).wait_send()
                if name != "s":
                    by_z(kind, name, g).wait_send()
    for m in range(2):
        for copy in (by_core(0, m), by_core(1, m), by_y(m)):
            copy.wait_send()
    for copy in [to_n, to_y, on_y] + to_c:
        copy.wait_send()
    for which in range(3):
        for i in range(len(order)):
            exchange(which, i).wait_send()


def local_lines(
    queries, keys, values, sink, stream, out_weight, norm_gain, gate_weight, up_weight, down_weight
):
    length = lax.axis_size("sp") // 2
    tokens = queries.shape[0]
    rows, model = stream.shape
    depth, wide = gate_weight.shape
    per = wide // LANES // 2
    tail = wide // 2 - per * LANES
    half = wide // 2
    slots = 2 * length
    part = down_weight.shape[1]
    blocks = tokens // WINDOW
    within, begins = turn_tables(slots * blocks + 2)
    vmem = pl.BlockSpec(memory_space=pltpu.VMEM)
    far = pl.BlockSpec(memory_space=pl.ANY)
    dma = pltpu.SemaphoreType.DMA
    dims = (length, tokens, rows, per, tail, tokens * slots)
    return pl.pallas_call(
        functools.partial(layer_kernel, dims),
        out_shape=jax.ShapeDtypeStruct((rows, model), BF),
        in_specs=[far] * 3 + [pl.BlockSpec(memory_space=pltpu.SMEM)] + [far] * 2 + [vmem] + [far] * 3 + [vmem] * 2,
        out_specs=vmem,
        scratch_shapes=[
            pltpu.VMEM(queries.shape, BF),
            pltpu.VMEM((tokens + 2 * WINDOW, 2 * LANES), BF),
            pltpu.VMEM((2, tokens + 2 * WINDOW, LANES), BF),
            pltpu.VMEM((2, tokens + 2 * WINDOW, LANES), BF),
            pltpu.VMEM(queries.shape, BF),
            pltpu.VMEM(out_weight.shape, BF),
            pltpu.VMEM(stream.shape, BF),
            pltpu.VMEM((2, depth, LANES), BF),
            pltpu.VMEM((depth, wide), BF),
            pltpu.VMEM((half, part), BF),
            pltpu.VMEM((slots, depth, wide), BF),
            pltpu.VMEM((slots, half, part), BF),
            pltpu.VMEM((2, rows, model), BF),
            pltpu.VMEM((2, rows, model), BF),
            pltpu.VMEM((2, 2, rows, model), F32),
            pltpu.VMEM((rows, model), BF),
            pltpu.VMEM((rows, model), BF),
            pltpu.VMEM((rows, model), BF),
            pltpu.VMEM((2, 4, rows, model), BF),
            pltpu.VMEM((2, 4 * rows, half), BF),
            pltpu.VMEM((slots, 4 * rows, part), BF),
            pltpu.VMEM((slots, 4 * rows, part), BF),
            pltpu.VMEM((slots, 4, rows, part), F32),
            pltpu.VMEM((slots, 2, rows, part), BF),
            pltpu.VMEM((slots, 2, rows, part), BF),
            pltpu.VMEM((slots, rows, part), BF),
            pltpu.VMEM((slots, rows, part), BF),
            dma((10,)), dma((2, 2)), dma((2, 2)),
            dma((2, 3, GCH)), dma((2, 4, GCH)), dma((slots, GCH)), dma((slots, DCH)),
            dma((3, 2)), dma((3, 2)), dma((7,)), dma((7,)), dma((3, slots)), dma((3, slots)),
        ],
        compiler_params=pltpu.CompilerParams(
            collective_id=0, has_side_effects=True, vmem_limit_bytes=63 * 1024 * 1024
        ),
    )(
        queries, keys, values, sink, stream, out_weight, norm_gain[None],
        gate_weight, up_weight, down_weight, jnp.asarray(within), jnp.asarray(begins),
    )


def solution(mesh):
    placed = (
        P("sp", "tp"),
        P("sp", "tp"),
        P("sp", "tp"),
        P("tp"),
        P(("sp", "tp"), None),
        P("tp", None),
        P(),
        P("sp", "tp"),
        P("sp", "tp"),
        P("tp", "sp"),
    )
    lines = mesh.shape["tp"] == 4 and mesh.shape["sp"] == 8
    return jax.shard_map(
        local_lines if lines else local, mesh=mesh, in_specs=placed, out_specs=P(("sp", "tp"), None), check_vma=False
    )
```
